32 devices in a mesh: sp: 16 (over z, y, x), tp: 2 (over core).
Axes of the slice: x: 2, y: 2, z: 4, core: 2. Of those that a mesh axis runs over, the one named last changes fastest.
Arguments:
- queries: bfloat16 [4096, 1024], P('sp', 'tp'), may hold values from -7 to 7
- keys: bfloat16 [4096, 256], P('sp', 'tp'), may hold values from -6 to 6
- values: bfloat16 [4096, 256], P('sp', 'tp'), may hold values from -6 to 6
- q_gain: float32 [64], replicated, may hold values from 0.5 to 5
- k_gain: float32 [64], replicated, may hold values from 0.5 to 5
- resid: bfloat16 [4096, 2048], P(('sp', 'tp')), may hold values from -6 to 6
- out_weight: bfloat16 [1024, 2048], P('tp'), may hold values from -0.1875 to 0.1875
- post_gain: float32 [2048], replicated, may hold values from 0.1 to 1.9
- ffn_gain: float32 [2048], replicated, may hold values from 0.1 to 1.9
- post_ffn_gain: float32 [2048], replicated, may hold values from 0.1 to 1.9
- gate_w: bfloat16 [16, 2048, 3584], P('sp', None, 'tp'), may hold values from -0.125 to 0.125
- up_w: bfloat16 [16, 2048, 3584], P('sp', None, 'tp'), may hold values from -0.125 to 0.125
- down_w: bfloat16 [16, 3584, 2048], P('sp', 'tp'), may hold values from -0.09375 to 0.09375
- route_ids: int32 [4096, 2], P(('sp', 'tp')), may hold values from 0 to 15, all different within a row; in each aligned block of 128 rows (0 to 127, 128 to 255, ...) at most 24 rows name the same one
- route_w: float32 [4096, 2], P(('sp', 'tp')), may hold values from 0.2 to 1
Outputs:
- layer_out: bfloat16 [4096, 2048], P(('sp', 'tp'))
The draws below stay inside these ranges and needn't reach their ends.
Inputs may be any that keep to these rules, and one draw needn't show every extreme that they name: `route_ids`: each row names 2 different experts. In each aligned block of 128 rows (the rows of one device) no expert is named more than 24 times, a bound that some blocks reach.
All inputs are finite; a program needn't handle non-finite values.
Results may differ from the reference program's by a relative error of at most 0.017.
The reference program's roundings to bfloat16 on the way count: a program that leaves them out, or rounds other values in their place, can miss the bound.
Values may be sent and summed in bfloat16 or wider, within the bound.
A program may use at most 128 MiB of HBM per device.

```python
import math
import jax
import jax.numpy as jnp
import numpy as np
from jax import lax

D = 2048
HEADS = 16
KV_HEADS = 4
HEAD_DIM = 64
FF_E = 3584
GRID_W = 64
TOP = 2
TOKENS = 4096
EXPERTS = 16
ROWS_DEV = 128
CAP = 24
N_SP = 16
N_TP = 2


def base_keys(key):
    fresh = jax.random.normal(jax.random.fold_in(key, 11), (TOKENS, KV_HEADS * HEAD_DIM), jnp.float32)
    return jnp.clip(fresh, -6.0, 6.0)


def draw_keys(key, part):
    return base_keys(key).astype(jnp.bfloat16)


def draw_queries(key, part):
    fresh = jax.random.normal(jax.random.fold_in(key, 12), (TOKENS, HEADS, HEAD_DIM), jnp.float32)
    fresh = jnp.clip(fresh, -6.0, 6.0)
    return fresh.reshape(TOKENS, HEADS * HEAD_DIM).astype(jnp.bfloat16)


def gain_draw(key, salt):
    spread = jax.random.uniform(jax.random.fold_in(key, salt), (HEAD_DIM,), jnp.float32, math.log(0.5), math.log(2.0))
    return jnp.exp(spread)


def draw_q_gain(key, part):
    return gain_draw(key, 13)


def draw_k_gain(key, part):
    return gain_draw(key, 14)


def levels(stream_key, extent, shards, smallest, largest):
    factor_of, own = 1.0, jax.random.fold_in(stream_key, 6)
    for position, blocks in shards:
        heights = jnp.exp(jax.random.uniform(jax.random.fold_in(own, position), (blocks,), jnp.float32, smallest / len(shards), largest / len(shards)))
        factor_of = factor_of * jnp.repeat(heights, extent[position] // blocks).reshape([-1 if axis == position else 1 for axis in range(len(extent))])
    return factor_of


def routed_block(rng, own, number, rows, count, top, reach, skew):
    ranking = jax.random.permutation(rng, count)
    heavy_load, common = portions_of(count, rows * top, reach, skew, True), portions_of(count, rows * top, reach, skew, False)
    places = jnp.arange(count)

    def named(lengths, turn):
        used = int((lengths > 0).sum())
        fixed = max(1, used // 4)
        shifted = fixed + (places - fixed + turn * (used - fixed)) % max(1, count - fixed)
        return jnp.zeros((count,), jnp.int32).at[ranking[jnp.where(places < fixed, places, shifted)]].set(jnp.asarray(lengths, jnp.int32))

    lengths = jnp.where(number % 4 == 0, named(heavy_load, number // 4), named(common, number - number // 4 - 1))
    mixed = jax.random.permutation(jax.random.fold_in(own, 3), count)
    source_of, receiver = mixed[0:count // 2 * 2:2], mixed[1:count // 2 * 2:2]
    slack = jnp.minimum(lengths[source_of] - 1, reach - lengths[receiver]) // 2
    slack = jnp.where((source_of == ranking[0]) | (receiver == ranking[0]) | (lengths[receiver] == 0), 0, jnp.maximum(slack, 0))
    shifted = jax.random.randint(jax.random.fold_in(own, 4), (count // 2,), 0, 1 << 20) % (slack + 1)
    lengths = lengths.at[source_of].add(-shifted).at[receiver].add(shifted)
    labels = jnp.searchsorted(jnp.cumsum(lengths), jnp.arange(rows * top), side="right").astype(jnp.int32)
    listing = labels.reshape(top, rows).T
    listing = listing[jax.random.permutation(jax.random.fold_in(own, 1), rows)]
    turn = jax.random.randint(jax.random.fold_in(own, 2), (rows, 1), 0, top)
    return jnp.take_along_axis(listing, (jnp.arange(top)[None, :] + turn) % top, axis=1)


def portions_of(amount, total, limit, slope, full):
    loads = [(1 << 20) // math.isqrt(standing ** slope) + 1 for standing in range(1, amount + 1)]
    largest = limit if full else min(limit, max(-(-total // amount), total * loads[0] // sum(loads)))
    least = 1 if total - largest >= amount - 1 else 0
    holding, rest = [largest] + [least] * (amount - 1), total - largest - least * (amount - 1)
    while rest > 0:
        candidates = [i for i in range(1, amount) if holding[i] < largest] or [i for i in range(1, amount) if holding[i] < limit]
        mass, remaining = sum([loads[i] for i in candidates]), rest
        for i in candidates:
            addition = min(limit - holding[i], max(1, remaining * loads[i] // mass), rest)
            holding[i] = holding[i] + addition
            rest = rest - addition
    return np.array(holding)


def noise(key, shape, deviation, most, cuts=(), held_as=jnp.bfloat16):
    array = jax.random.normal(key, shape, jnp.float32) * deviation
    if len(cuts) > 0:
        array = levels(key, shape, cuts, -0.22, 0.18) * array
    return jnp.clip(array, min=-most, max=most).astype(held_as)


def setup_inputs(seed: int = 0) -> dict:
    streams_of = jax.random.split(jax.random.key(seed), 16)
    queries = draw_queries(jax.random.fold_in(streams_of[15], 71), 0)
    keys = draw_keys(jax.random.fold_in(streams_of[15], 71), 0)
    values = noise(streams_of[2], (TOKENS, KV_HEADS * HEAD_DIM), 1.0, 6.0, ((0, 16), (1, 2)))
    q_gain = draw_q_gain(jax.random.fold_in(streams_of[15], 71), 0)
    k_gain = draw_k_gain(jax.random.fold_in(streams_of[15], 71), 0)
    resid = noise(streams_of[5], (TOKENS, D), 1.0, 6.0, ((0, 32),))
    out_weight = noise(streams_of[6], (HEADS * HEAD_DIM, D), (HEADS * HEAD_DIM) ** -0.5, 0.1875, ((0, 2),))
    post_gain = jnp.clip(1.0 + 0.18 * jax.random.normal(streams_of[7], (D,), jnp.float32), 0.1, 1.9)
    ffn_gain = jnp.clip(1.0 + 0.18 * jax.random.normal(streams_of[8], (D,), jnp.float32), 0.1, 1.9)
    post_ffn_gain = jnp.clip(1.0 + 0.18 * jax.random.normal(streams_of[9], (D,), jnp.float32), 0.1, 1.9)
    gate_w = noise(streams_of[10], (EXPERTS, D, FF_E), D ** -0.5, 0.125, ((0, 16), (2, 2)))
    up_w = noise(streams_of[11], (EXPERTS, D, FF_E), D ** -0.5, 0.125, ((0, 16), (2, 2)))
    down_w = noise(streams_of[12], (EXPERTS, FF_E, D), FF_E ** -0.5, 0.09375, ((0, 16), (1, 2)))
    route_ids_keys = jax.random.split(jax.random.fold_in(streams_of[13], 1), TOKENS // ROWS_DEV)
    route_ids_turns = jax.random.permutation(jax.random.fold_in(streams_of[13], 3), TOKENS // ROWS_DEV)
    route_ids = jax.vmap(lambda own, number: routed_block(jax.random.fold_in(streams_of[13], 2), own, number, ROWS_DEV, EXPERTS, TOP, CAP, 1))(route_ids_keys, route_ids_turns).reshape((TOKENS, TOP))
    route_w = jnp.clip(0.2 + 0.8 * jax.random.uniform(streams_of[14], (TOKENS, TOP), jnp.float32) ** levels(streams_of[14], (TOKENS, TOP), ((0, 32),), -0.2, 0.2), 0.2, 1.0)
    return dict(queries=queries, keys=keys, values=values, q_gain=q_gain, k_gain=k_gain, resid=resid, out_weight=out_weight, post_gain=post_gain, ffn_gain=ffn_gain, post_ffn_gain=post_ffn_gain, gate_w=gate_w, up_w=up_w, down_w=down_w, route_ids=route_ids, route_w=route_w)


EPS = 1e-06
THETA = 10000.0

def qk_prepare(raw, gain, positions, head_count):
    count_rows = raw.shape[0]
    values32 = raw.astype(jnp.float32).reshape(count_rows, head_count, HEAD_DIM)
    normed = values32 * lax.rsqrt(lax.optimization_barrier(jnp.mean(values32 * values32, axis=-1, keepdims=True)) + EPS) * gain
    half_dim = HEAD_DIM // 2
    freqs = THETA ** (-jnp.arange(0, half_dim, 2, dtype=jnp.float32) / half_dim)
    grid_row = (positions // GRID_W).astype(jnp.float32)
    grid_col = (positions % GRID_W).astype(jnp.float32)
    angles = jnp.concatenate([grid_row[:, None] * freqs, grid_col[:, None] * freqs], axis=-1)
    cosine = jnp.cos(angles)[:, None, :]
    sine = jnp.sin(angles)[:, None, :]
    paired = normed.reshape(count_rows, head_count, half_dim, 2)
    first = paired[..., 0]
    second = paired[..., 1]
    turned = jnp.stack([first * cosine - second * sine, first * sine + second * cosine], axis=-1)
    return turned.reshape(count_rows, head_count * HEAD_DIM).astype(jnp.bfloat16)

def rms_scale(values32, gain):
    return values32 * lax.rsqrt(lax.optimization_barrier(jnp.mean(values32 * values32, axis=-1, keepdims=True)) + EPS) * gain

def reference(queries, keys, values, q_gain, k_gain, resid, out_weight, post_gain, ffn_gain, post_ffn_gain, gate_w, up_w, down_w, route_ids, route_w):
    positions = jnp.arange(TOKENS, dtype=jnp.int32)
    group_size = HEADS // KV_HEADS
    scale_factor = HEAD_DIM ** (-0.5)
    query_n = qk_prepare(queries, q_gain, positions, HEADS).reshape(TOKENS // 128, 128, KV_HEADS, group_size, HEAD_DIM)
    key_n = qk_prepare(keys, k_gain, positions, KV_HEADS).reshape(TOKENS, KV_HEADS, HEAD_DIM).astype(jnp.float32)
    value_n = values.reshape(TOKENS, KV_HEADS, HEAD_DIM).astype(jnp.float32)

    def attend(block):
        scores = jnp.einsum('qhgd,khd->hgqk', block.astype(jnp.float32), key_n) * scale_factor
        top_score = lax.optimization_barrier(jnp.max(scores, axis=-1, keepdims=True))
        expo = jnp.exp(scores - top_score)
        total = lax.optimization_barrier(jnp.sum(expo, axis=-1))
        weights = lax.optimization_barrier(expo.astype(jnp.bfloat16)).astype(jnp.float32)
        summed = jnp.einsum('hgqk,khd->qhgd', weights, value_n)
        result = summed / jnp.transpose(total, (2, 0, 1))[..., None]
        return result.astype(jnp.bfloat16).reshape(128, HEADS * HEAD_DIM)
    attended = lax.map(attend, query_n).reshape(TOKENS, HEADS * HEAD_DIM)
    mixed = jnp.dot(attended, out_weight, preferred_element_type=jnp.float32)
    hidden_state = (resid.astype(jnp.float32) + rms_scale(mixed, post_gain)).astype(jnp.bfloat16)
    normed = rms_scale(hidden_state.astype(jnp.float32), ffn_gain).astype(jnp.bfloat16)
    bound = CAP * N_SP * N_TP
    pair_count = TOKENS * TOP
    pair_experts = route_ids.reshape(-1)
    padded_rows = jnp.concatenate([normed, jnp.zeros((1, D), jnp.bfloat16)], axis=0)
    part_width = FF_E // N_TP

    def expert_pass(expert):
        slots = jnp.nonzero(pair_experts == expert, size=bound, fill_value=pair_count)[0].astype(jnp.int32)
        token_ids = jnp.where(slots < pair_count, slots // TOP, TOKENS).astype(jnp.int32)
        rows_in = padded_rows[token_ids]
        gate = jnp.dot(rows_in, gate_w[expert], preferred_element_type=jnp.float32)
        upward = jnp.dot(rows_in, up_w[expert], preferred_element_type=jnp.float32)
        inner = (jax.nn.silu(gate) * upward).astype(jnp.bfloat16)
        down_here = down_w[expert]
        total = jnp.zeros((bound, D), jnp.float32)
        for part in range(N_TP):
            partial_sum = jnp.dot(inner[:, part * part_width:(part + 1) * part_width], down_here[part * part_width:(part + 1) * part_width], preferred_element_type=jnp.float32)
            total = total + lax.optimization_barrier(partial_sum.astype(jnp.bfloat16)).astype(jnp.float32)
        return (slots, total.astype(jnp.bfloat16))
    slot_table, results = lax.map(expert_pass, jnp.arange(EXPERTS, dtype=jnp.int32))
    placed = jnp.zeros((pair_count + 1, D), jnp.bfloat16).at[slot_table.reshape(-1)].set(results.reshape(-1, D))
    picked = placed[:pair_count].reshape(TOKENS, TOP, D).astype(jnp.float32)
    combined = lax.optimization_barrier(jnp.sum(route_w[:, :, None] * picked, axis=1))
    return (hidden_state.astype(jnp.float32) + rms_scale(combined, post_ffn_gain)).astype(jnp.bfloat16)
```

```python
import functools

import jax
import jax.numpy as jnp
from jax import lax
from jax.experimental import pallas as pl
from jax.experimental.pallas import tpu as pltpu
from jax.sharding import PartitionSpec as P

HEAD_DIM = 64
GRID_W = 64


EPS = 1e-06
THETA = 10000.0


LANES = 128
EXP2_SCALE = HEAD_DIM ** (-0.5) * 1.4426950408889634
MESH = pl.DeviceIdType.MESH


def turn_tables(positions):
    lane = jnp.arange(LANES, dtype=jnp.int32) % HEAD_DIM
    pair = lane // 2
    quarter = HEAD_DIM // 4
    freqs = THETA ** (-2.0 * (pair % quarter).astype(jnp.float32) / (HEAD_DIM // 2))
    grid_row = (positions // GRID_W).astype(jnp.float32)[:, None]
    grid_col = (positions % GRID_W).astype(jnp.float32)[:, None]
    angles = jnp.where(pair < quarter, grid_row, grid_col) * freqs
    sign = jnp.where(lane % 2 == 0, -1.0, 1.0)
    return jnp.cos(angles), jnp.sin(angles) * sign


def prep_kernel(q_ref, k_ref, v_ref, gains_ref, cos_ref, sin_ref, qz_ref, pay_ref):
    tok = q_ref.shape[0]
    heads = q_ref.shape[1] // HEAD_DIM
    group = heads // (k_ref.shape[1] // HEAD_DIM)
    row = lax.broadcasted_iota(jnp.int32, (LANES, LANES), 0) // HEAD_DIM
    col = lax.broadcasted_iota(jnp.int32, (LANES, LANES), 1) // HEAD_DIM
    mean_mat = jnp.where(row == col, 1.0 / HEAD_DIM, 0.0).astype(jnp.float32)
    even = lax.broadcasted_iota(jnp.int32, (tok, LANES), 1) % 2 == 0
    cosine = cos_ref[...]
    sine = sin_ref[...]

    def turned(raw, gain):
        x = raw.astype(jnp.float32)
        mean = jnp.dot(
            x * x, mean_mat, precision=lax.Precision.HIGHEST, preferred_element_type=jnp.float32
        )
        normed = x * lax.rsqrt(mean + EPS) * gain
        swapped = jnp.where(even, pltpu.roll(normed, LANES - 1, 1), pltpu.roll(normed, 1, 1))
        return normed * cosine + swapped * sine

    qz_ref[...] = jnp.zeros(qz_ref.shape, qz_ref.dtype)
    for tile in range(q_ref.shape[1] // LANES):
        out = turned(q_ref[:, tile * LANES : (tile + 1) * LANES], gains_ref[0:1, :])
        flipped = out.T.astype(jnp.bfloat16)
        for part in range(LANES // HEAD_DIM):
            head = tile * (LANES // HEAD_DIM) + part
            base = (head // group) * HEAD_DIM
            qz_ref[head, base : base + HEAD_DIM, :] = flipped[
                part * HEAD_DIM : (part + 1) * HEAD_DIM
            ]
    pay_ref[0:tok, :] = turned(k_ref[...], gains_ref[1:2, :]).astype(jnp.bfloat16)
    for tile in range(tok // LANES):
        block = v_ref[tile * LANES : (tile + 1) * LANES, :].astype(jnp.float32)
        pay_ref[tok + tile * LANES : tok + (tile + 1) * LANES, :] = block.T.astype(jnp.bfloat16)


def attend_kernel(
    count, group, qz_ref, pay_ref, out_ref, held, run_max, run_sum, run_acc, send_sem, recv_sem
):
    me = lax.axis_index("sp")
    heads = qz_ref.shape[0]
    tok = qz_ref.shape[2]

    barrier = pltpu.get_barrier_semaphore()
    for step in range(1, count):
        pl.semaphore_signal(
            barrier, inc=1, device_id={"sp": lax.rem(me + step, count)}, device_id_type=MESH
        )
    pl.semaphore_wait(barrier, count - 1)

    def send(step):
        return pltpu.make_async_remote_copy(
            src_ref=pay_ref,
            dst_ref=held.at[me],
            send_sem=send_sem.at[step],
            recv_sem=recv_sem.at[me],
            device_id={"sp": lax.rem(me + step, count)},
            device_id_type=MESH,
        )

    for step in range(1, count):
        send(step).start()

    def block(keys, values_t, first):
        for head in range(heads):
            base = (head // group) * HEAD_DIM
            rows = pl.ds(head * HEAD_DIM, HEAD_DIM)
            one = pl.ds(head, 1)
            scores = jnp.dot(keys, qz_ref[head], preferred_element_type=jnp.float32)
            top = jnp.max(scores, axis=0, keepdims=True)
            if not first:
                old = run_max[one, :]
                top = jnp.maximum(old, top)
            expo = jnp.exp2((scores - top) * EXP2_SCALE)
            total = jnp.sum(expo, axis=0, keepdims=True)
            added = jnp.dot(
                values_t[base : base + HEAD_DIM],
                expo.astype(jnp.bfloat16),
                preferred_element_type=jnp.float32,
            )
            if not first:
                shrink = jnp.exp2((old - top) * EXP2_SCALE)
                total = total + run_sum[one, :] * shrink
                added = added + run_acc[rows, :] * shrink
            run_max[one, :] = top
            run_sum[one, :] = total
            run_acc[rows, :] = added

    def split(ref):
        tiles = [ref[tok + t * LANES : tok + (t + 1) * LANES, :] for t in range(tok // LANES)]
        return ref[0:tok, :], jnp.concatenate(tiles, axis=1)

    block(*split(pay_ref), True)

    @pl.loop(1, count)
    def _(step):
        owner = lax.rem(me - step + count, count)
        pltpu.make_async_copy(held.at[owner], held.at[owner], recv_sem.at[owner]).wait()
        block(*split(held.at[owner]), False)

    for head in range(0, heads, LANES // HEAD_DIM):
        parts = []
        for h in range(head, head + LANES // HEAD_DIM):
            rows = pl.ds(h * HEAD_DIM, HEAD_DIM)
            parts.append(run_acc[rows, :] / run_sum[pl.ds(h, 1), :])
        both = jnp.concatenate(parts, axis=0)
        out_ref[:, head * HEAD_DIM : head * HEAD_DIM + LANES] = both.T.astype(jnp.bfloat16)
    for step in range(1, count):
        send(step).wait_send()


def attention(queries, keys, values, q_gain, k_gain):
    tok = queries.shape[0]
    sp_count = lax.axis_size("sp")
    heads = queries.shape[1] // HEAD_DIM
    kv_heads = keys.shape[1] // HEAD_DIM
    positions = lax.axis_index("sp") * tok + jnp.arange(tok, dtype=jnp.int32)
    cosine, sine = turn_tables(positions)
    gains = jnp.tile(jnp.stack([q_gain, k_gain]), (1, LANES // HEAD_DIM))
    vmem = pl.BlockSpec(memory_space=pltpu.VMEM)
    qz, payload = pl.pallas_call(
        prep_kernel,
        out_shape=(
            jax.ShapeDtypeStruct((heads, LANES, tok), jnp.bfloat16),
            jax.ShapeDtypeStruct((2 * tok, LANES), jnp.bfloat16),
        ),
        in_specs=[vmem] * 6,
        out_specs=(vmem, vmem),
        name="prep",
    )(queries, keys, values, gains, cosine, sine)
    return pl.pallas_call(
        functools.partial(attend_kernel, sp_count, heads // kv_heads),
        out_shape=jax.ShapeDtypeStruct((tok, heads * HEAD_DIM), jnp.bfloat16),
        in_specs=[vmem] * 2,
        out_specs=vmem,
        scratch_shapes=[
            pltpu.VMEM((sp_count, 2 * tok, LANES), jnp.bfloat16),
            pltpu.VMEM((heads, tok), jnp.float32),
            pltpu.VMEM((heads, tok), jnp.float32),
            pltpu.VMEM((heads * HEAD_DIM, tok), jnp.float32),
            pltpu.SemaphoreType.DMA((sp_count,)),
            pltpu.SemaphoreType.DMA((sp_count,)),
        ],
        compiler_params=pltpu.CompilerParams(collective_id=0, has_side_effects=True),
        cost_estimate=pl.CostEstimate(
            flops=4 * sp_count * tok * tok * heads * HEAD_DIM,
            bytes_accessed=4 * sp_count * tok * LANES,
            transcendentals=sp_count * tok * tok * heads,
        ),
        name="attend",
    )(qz, payload)


def rms_scale(values32, gain):
    return values32 * lax.rsqrt(jnp.mean(values32 * values32, axis=-1, keepdims=True) + EPS) * gain


def per_device(
    queries,
    keys,
    values,
    q_gain,
    k_gain,
    resid,
    out_weight,
    post_gain,
    ffn_gain,
    post_ffn_gain,
    gate_w,
    up_w,
    down_w,
    route_ids,
    route_w,
):
    tok_local = queries.shape[0]
    width = resid.shape[1]
    tp_count = lax.axis_size("tp")
    sp_count = lax.axis_size("sp")
    attended = attention(queries, keys, values, q_gain, k_gain)
    row_count = tok_local // tp_count
    token_heads = lax.all_to_all(attended, "tp", split_axis=0, concat_axis=1, tiled=True)
    mixed = jnp.dot(
        token_heads,
        lax.all_gather(out_weight, "tp", axis=0, tiled=True),
        preferred_element_type=jnp.float32,
    )
    hidden_state = (resid.astype(jnp.float32) + rms_scale(mixed, post_gain)).astype(jnp.bfloat16)
    normed = rms_scale(hidden_state.astype(jnp.float32), ffn_gain).astype(jnp.bfloat16)
    top_count = route_ids.shape[1]
    expert_count = gate_w.shape[0] * sp_count
    capacity = 3 * tok_local * top_count // (2 * tp_count * expert_count)
    flat_routes = route_ids.reshape(-1)
    chosen = (flat_routes[:, None] == jnp.arange(expert_count, dtype=jnp.int32)[None, :]).astype(
        jnp.int32
    )
    earlier = jnp.cumsum(chosen, axis=0) - chosen
    ranks = jnp.sum(earlier * chosen, axis=1)
    slot_ids = flat_routes * capacity + ranks
    slot_range = jnp.arange(expert_count * capacity, dtype=jnp.int32)
    selector = jnp.sum(
        (slot_ids.reshape(row_count, top_count)[:, :, None] == slot_range[None, None, :]).astype(
            jnp.bfloat16
        ),
        axis=1,
    )
    outgoing = lax.dot_general(
        selector, normed, (((0,), (0,)), ((), ())), preferred_element_type=jnp.float32
    )
    outgoing = outgoing.astype(jnp.bfloat16).reshape(expert_count, capacity, width)
    arrived = lax.all_to_all(outgoing, "sp", split_axis=0, concat_axis=0, tiled=True)
    flat_rows = lax.all_gather(arrived, "tp", axis=0, tiled=True).reshape(-1, width)
    gate = jnp.dot(flat_rows, gate_w[0], preferred_element_type=jnp.float32)
    upward = jnp.dot(flat_rows, up_w[0], preferred_element_type=jnp.float32)
    inner = (jax.nn.silu(gate) * upward).astype(jnp.bfloat16)
    expert_out = lax.psum_scatter(
        jnp.dot(inner, down_w[0], preferred_element_type=jnp.float32).astype(jnp.bfloat16),
        "tp",
        scatter_dimension=0,
        tiled=True,
    )
    returned = lax.all_to_all(
        expert_out.reshape(expert_count, capacity, width),
        "sp",
        split_axis=0,
        concat_axis=0,
        tiled=True,
    )
    picked = returned.reshape(expert_count * capacity, width)[slot_ids]
    picked = picked.reshape(row_count, top_count, width).astype(jnp.float32)
    combined = jnp.sum(route_w[:, :, None] * picked, axis=1)
    return (hidden_state.astype(jnp.float32) + rms_scale(combined, post_ffn_gain)).astype(
        jnp.bfloat16
    )


def solution(mesh):
    in_specs = (
        P("sp", "tp"),
        P("sp", "tp"),
        P("sp", "tp"),
        P(),
        P(),
        P(("sp", "tp"), None),
        P("tp", None),
        P(),
        P(),
        P(),
        P("sp", None, "tp"),
        P("sp", None, "tp"),
        P("sp", "tp", None),
        P(("sp", "tp"), None),
        P(("sp", "tp"), None),
    )
    out_specs = P(("sp", "tp"), None)
    return jax.shard_map(
        per_device, mesh=mesh, in_specs=in_specs, out_specs=out_specs, check_vma=False
    )
```
